32 devices in a mesh: grp: 2 (over y), sp: 4 (over z), tp: 4 (over x, core).
Axes of the slice: x: 2, y: 2, z: 4, core: 2. Of those that a mesh axis runs over, the one named last changes fastest.
Arguments:
- tokens: bfloat16 [2048, 4096], P(('grp', 'sp')), parts along dimension 0, may hold values from -6 to 6
- norm_gain: bfloat16 [2, 4096], replicated, may hold values from 0.099609375 to 1.8984375
- w_query: bfloat16 [2, 4096, 2048], P(None, 'sp', 'tp'), may hold values from -0.09375 to 0.09375
- w_key: bfloat16 [2, 4096, 2048], P(None, 'sp', 'tp'), may hold values from -0.09375 to 0.09375
- w_value: bfloat16 [2, 4096, 2048], P(None, 'sp', 'tp'), may hold values from -0.09375 to 0.09375
- w_out: bfloat16 [2, 2048, 4096], P(None, 'tp', 'sp'), may hold values from -0.125 to 0.125
- offset_bias: float32 [2, 16, 15, 31], P(None, 'tp'), may hold values from -4 to 300
Outputs:
- mixed: bfloat16 [2048, 4096], P(('grp', 'sp')), parts along dimension 0
The draws below stay inside these ranges and needn't reach their ends.
There are 2 independent parts, one for each index of `grp`. The reference program is written for one: setup_inputs(seed, part) draws one part's arguments, and reference() takes and returns one part's arrays. A program takes and returns all parts, laid end to end along the dimension named above; an argument that names none is the same for every part. Nothing has to cross between parts.
All inputs are finite; a program needn't handle non-finite values.
Results may differ from the reference program's by a relative error of at most 0.013.
Values may be sent and summed in bfloat16 or wider, within the bound.
A program may use at most 128 MiB of HBM per device.

```python
import jax
import jax.numpy as jnp
from jax import lax

D = 4096
HEADS = 16
HD = 128
GRID_W = 64
KR = 8
KC = 16
LAYERS = 2
ROWS_DEV = 4
TOKENS = 1024
N_SP = 4
N_TP = 4


def draw_offset_bias(key, part):
    shape = (LAYERS, HEADS, 2 * KR - 1, 2 * KC - 1)
    first_key, second_key = jax.random.split(jax.random.fold_in(key, 17))
    base = jnp.clip(jax.random.normal(first_key, shape, jnp.float32), -4.0, 4.0)
    return base


def steps_of(key, shape, shards, least, largest):
    factor_of, own = 1.0, jax.random.fold_in(key, 6)
    for position, parts in shards:
        heights = jnp.exp(jax.random.uniform(jax.random.fold_in(own, position), (parts,), jnp.float32, least / len(shards), largest / len(shards)))
        factor_of = factor_of * jnp.repeat(heights, shape[position] // parts).reshape([-1 if axis == position else 1 for axis in range(len(shape))])
    return factor_of


def scatter_about(own_key, dims, scale, most, pieces=(), kind=jnp.bfloat16):
    values = jax.random.normal(own_key, dims, jnp.float32) * scale
    if len(pieces) > 0:
        values = steps_of(own_key, dims, pieces, -0.22, 0.18) * values
    return jnp.clip(values, min=-most, max=most).astype(kind)


def setup_inputs(seed: int = 0, part: int = 0) -> dict:
    key_list = jax.random.split(jax.random.key(seed), 8)
    part_keys = jax.random.split(jax.random.fold_in(key_list[7], part), 8)
    tokens = scatter_about(part_keys[0], (TOKENS, D), 1.0, 6.0, ((0, 4),))
    norm_gain = jnp.clip(1.0 + 0.18 * jax.random.normal(key_list[1], (LAYERS, D), jnp.float32), 0.099609375, 1.8984375).astype(jnp.bfloat16)
    w_query = scatter_about(key_list[2], (LAYERS, D, HEADS * HD), D ** -0.5, 0.09375, ((1, 4), (2, 4)))
    w_key = scatter_about(key_list[3], (LAYERS, D, HEADS * HD), D ** -0.5, 0.09375, ((1, 4), (2, 4)))
    w_value = scatter_about(key_list[4], (LAYERS, D, HEADS * HD), D ** -0.5, 0.09375, ((1, 4), (2, 4)))
    w_out = scatter_about(key_list[5], (LAYERS, HEADS * HD, D), (HEADS * HD) ** -0.5, 0.125, ((1, 4), (2, 4)))
    offset_bias = draw_offset_bias(jax.random.fold_in(key_list[7], 71), part)
    return dict(tokens=tokens, norm_gain=norm_gain, w_query=w_query, w_key=w_key, w_value=w_value, w_out=w_out, offset_bias=offset_bias)


norm_eps = 1e-06

def rms_rows(values, gain):
    wide = values.astype(jnp.float32)
    scaled = wide * lax.rsqrt(lax.optimization_barrier(jnp.mean(wide * wide, axis=-1, keepdims=True)) + norm_eps)
    return (scaled * gain.astype(jnp.float32)).astype(jnp.bfloat16)

def reference(tokens, norm_gain, w_query, w_key, w_value, w_out, offset_bias):
    grid_rows = ROWS_DEV * N_SP
    group_width = HEADS // N_TP * HD
    scale = HD ** (-0.5)
    columns = jnp.arange(GRID_W, dtype=jnp.int32)
    col_first = jnp.clip(columns - KC // 2, 0, GRID_W - KC)
    col_inside = (columns[None, :] >= col_first[:, None]) & (columns[None, :] < col_first[:, None] + KC)
    col_offset = jnp.clip(columns[None, :] - columns[:, None], 1 - KC, KC - 1) + KC - 1
    row_first = jnp.clip(jnp.arange(grid_rows, dtype=jnp.int32) - KR // 2, 0, grid_rows - KR)
    residual = tokens
    for layer_index in range(LAYERS):
        normed = rms_rows(residual, norm_gain[layer_index])
        queries = jnp.dot(normed, w_query[layer_index], preferred_element_type=jnp.float32).astype(jnp.bfloat16)
        keys = jnp.dot(normed, w_key[layer_index], preferred_element_type=jnp.float32).astype(jnp.bfloat16)
        values = jnp.dot(normed, w_value[layer_index], preferred_element_type=jnp.float32).astype(jnp.bfloat16)
        queries = queries.reshape(grid_rows, GRID_W, HEADS, HD)
        keys = keys.reshape(grid_rows, GRID_W, HEADS, HD)
        values = values.reshape(grid_rows, GRID_W, HEADS, HD)
        col_bias = offset_bias[layer_index].astype(jnp.float32)[:, :, col_offset]

        def attend_row(packed, keys=keys, values=values, col_bias=col_bias):
            row_index, row_queries = packed
            row_begin = row_first[row_index].astype(jnp.int32)
            row_keys = lax.dynamic_slice_in_dim(keys, row_begin, KR, 0).astype(jnp.float32)
            row_values = lax.dynamic_slice_in_dim(values, row_begin, KR, 0).astype(jnp.float32)
            picked = row_begin + jnp.arange(KR, dtype=jnp.int32) - row_index + KR - 1
            bias = jnp.transpose(col_bias[:, picked], (0, 2, 1, 3))
            scores = jnp.einsum('qhd,jkhd->hqjk', row_queries.astype(jnp.float32), row_keys) * scale + bias
            scores = jnp.where(col_inside[None, :, None, :], scores, -jnp.inf)
            weights = jax.nn.softmax(scores.reshape(HEADS, GRID_W, KR * GRID_W), axis=-1).astype(jnp.bfloat16)
            weights = lax.optimization_barrier(weights)
            weights = weights.reshape(HEADS, GRID_W, KR, GRID_W).astype(jnp.float32)
            return jnp.einsum('hqjk,jkhd->qhd', weights, row_values).astype(jnp.bfloat16)
        attended = lax.map(attend_row, (jnp.arange(grid_rows, dtype=jnp.int32), queries))
        attended = attended.reshape(grid_rows * GRID_W, HEADS * HD)
        branch = jnp.zeros(residual.shape, jnp.float32)
        for group_index in range(N_TP):
            lower = group_index * group_width
            rounded = jnp.dot(attended[:, lower:lower + group_width], w_out[layer_index][lower:lower + group_width], preferred_element_type=jnp.float32).astype(jnp.bfloat16)
            branch = branch + lax.optimization_barrier(rounded).astype(jnp.float32)
        residual = (residual.astype(jnp.float32) + branch).astype(jnp.bfloat16)
    return residual
```

```python
import jax
import jax.numpy as jnp
from jax import lax
from jax.sharding import PartitionSpec as P

HD = 128
GRID_W = 64
KR = 8
KC = 16
LAYERS = 2


norm_eps = 1e-06


def with_halo(block, sides, width):
    for axis, dim in sides:
        count = lax.axis_size(axis)
        forward = [(i, i + 1) for i in range(count - 1)]
        backward = [(target, source) for source, target in forward]
        low = lax.ppermute(
            lax.slice_in_dim(block, block.shape[dim] - width, None, axis=dim), axis, forward
        )
        high = lax.ppermute(lax.slice_in_dim(block, 0, width, axis=dim), axis, backward)
        block = jnp.concatenate([low, block, high], axis=dim)
    return block


def rms_rows(values, gain):
    wide = values.astype(jnp.float32)
    scaled = wide * lax.rsqrt(jnp.mean(wide * wide, axis=-1, keepdims=True) + norm_eps)
    return (scaled * gain.astype(jnp.float32)).astype(jnp.bfloat16)


def on_device(tokens, norm_gain, w_query, w_key, w_value, w_out, offset_bias):
    sp_count = lax.axis_size("sp")
    sp_index = lax.axis_index("sp")
    tok_rows = tokens.shape[0]
    local_rows = tok_rows // GRID_W
    grid_rows = local_rows * sp_count
    heads_here = offset_bias.shape[1]
    head_width = heads_here * HD
    reach = KR // 2
    scale = HD ** (-0.5)
    columns = jnp.arange(GRID_W, dtype=jnp.int32)
    col_first = jnp.clip(columns - KC // 2, 0, GRID_W - KC)
    col_inside = (columns[None, :] >= col_first[:, None]) & (
        columns[None, :] < col_first[:, None] + KC
    )
    col_offset = jnp.clip(columns[None, :] - columns[:, None], 1 - KC, KC - 1) + KC - 1
    col_onehot = (
        jnp.arange(2 * KC - 1, dtype=jnp.int32)[:, None, None] == col_offset[None, :, :]
    ).astype(jnp.float32)
    first_row = sp_index * local_rows
    own_rows = first_row + jnp.arange(local_rows, dtype=jnp.int32)
    row_first = jnp.clip(own_rows - reach, 0, grid_rows - KR)
    band_start = row_first - first_row + reach
    row_offset = (
        row_first[:, None] + jnp.arange(KR, dtype=jnp.int32)[None, :] - own_rows[:, None] + KR - 1
    )
    row_onehot = (
        row_offset[:, :, None] == jnp.arange(2 * KR - 1, dtype=jnp.int32)[None, None, :]
    ).astype(jnp.float32)
    qkv_weight = jnp.concatenate([w_query, w_key, w_value], axis=2)
    residual = lax.all_to_all(tokens, "sp", split_axis=1, concat_axis=0, tiled=True)
    width = residual.shape[1]
    features = width * sp_count
    for layer_index in range(LAYERS):
        wide = residual.astype(jnp.float32)
        squares = lax.psum_scatter(
            jnp.sum(wide * wide, axis=-1, keepdims=True), "sp", scatter_dimension=0, tiled=True
        )
        inverse = lax.rsqrt(squares / features + norm_eps)
        gain = lax.dynamic_slice_in_dim(norm_gain[layer_index], sp_index * width, width, 0)
        gained = (wide * gain.astype(jnp.float32)).astype(jnp.bfloat16)
        partial = jnp.dot(gained, qkv_weight[layer_index], preferred_element_type=jnp.float32)
        mine = lax.psum_scatter(
            partial.astype(jnp.bfloat16), "sp", scatter_dimension=0, tiled=True
        )
        mine = (mine.astype(jnp.float32) * inverse).astype(jnp.bfloat16)
        queries = mine[:, :head_width].reshape(local_rows, GRID_W, heads_here, HD)
        key_values = mine[:, head_width:].reshape(local_rows, GRID_W, 2 * head_width)
        padded = with_halo(key_values, (("sp", 0),), reach)
        bands = jax.vmap(lambda band_begin: lax.dynamic_slice_in_dim(padded, band_begin, KR, 0))(
            band_start
        )
        band_keys = bands[..., :head_width].reshape(local_rows, KR, GRID_W, heads_here, HD)
        band_values = bands[..., head_width:].reshape(local_rows, KR, GRID_W, heads_here, HD)
        col_bias = jnp.einsum(
            "hro,oqk->hrqk", offset_bias[layer_index], col_onehot, precision=lax.Precision.HIGHEST
        )
        full_bias = jnp.einsum(
            "ijr,hrqk->hiqjk", row_onehot, col_bias, precision=lax.Precision.HIGHEST
        )
        scores = jnp.einsum(
            "iqhd,ijkhd->hiqjk", queries, band_keys, preferred_element_type=jnp.float32
        )
        scores = scores * scale + full_bias
        scores = jnp.where(col_inside[None, None, :, None, :], scores, -jnp.inf)
        flattened = scores.reshape(heads_here, local_rows, GRID_W, KR * GRID_W)
        weights = jax.nn.softmax(flattened, axis=-1).astype(jnp.bfloat16)
        weights = weights.reshape(heads_here, local_rows, GRID_W, KR, GRID_W)
        attended = jnp.einsum(
            "hiqjk,ijkhd->iqhd", weights, band_values, preferred_element_type=jnp.float32
        )
        attended = attended.astype(jnp.bfloat16).reshape(tok_rows, head_width)
        every = lax.all_gather(attended, "sp", axis=0, tiled=True)
        share = jnp.dot(every, w_out[layer_index], preferred_element_type=jnp.float32)
        branch = lax.psum(share.astype(jnp.bfloat16), "tp").astype(jnp.float32)
        residual = (residual.astype(jnp.float32) + branch).astype(jnp.bfloat16)
    return lax.all_to_all(residual, "sp", split_axis=0, concat_axis=1, tiled=True)


def solution(mesh):
    return jax.shard_map(
        on_device,
        mesh=mesh,
        in_specs=(
            P(("grp", "sp"), None),
            P(),
            P(None, "sp", "tp"),
            P(None, "sp", "tp"),
            P(None, "sp", "tp"),
            P(None, "tp", "sp"),
            P(None, "tp", None, None),
        ),
        out_specs=P(("grp", "sp"), None),
        check_vma=False,
    )
```

```python
import functools

import jax
import jax.numpy as jnp
from jax import lax
from jax.experimental import pallas as pl
from jax.experimental.pallas import tpu as pltpu
from jax.sharding import PartitionSpec as P

HD = 128
GRID_W = 64
KR = 8
KC = 16
LAYERS = 2


norm_eps = 1e-06


def with_halo(block, sides, width):
    for axis, dim in sides:
        count = lax.axis_size(axis)
        forward = [(i, i + 1) for i in range(count - 1)]
        backward = [(target, source) for source, target in forward]
        low = lax.ppermute(
            lax.slice_in_dim(block, block.shape[dim] - width, None, axis=dim), axis, forward
        )
        high = lax.ppermute(lax.slice_in_dim(block, 0, width, axis=dim), axis, backward)
        block = jnp.concatenate([low, block, high], axis=dim)
    return block


def rms_rows(values, gain):
    wide = values.astype(jnp.float32)
    scaled = wide * lax.rsqrt(jnp.mean(wide * wide, axis=-1, keepdims=True) + norm_eps)
    return (scaled * gain.astype(jnp.float32)).astype(jnp.bfloat16)


def general(tokens, norm_gain, w_query, w_key, w_value, w_out, offset_bias):
    sp_count = lax.axis_size("sp")
    sp_index = lax.axis_index("sp")
    tok_rows = tokens.shape[0]
    local_rows = tok_rows // GRID_W
    grid_rows = local_rows * sp_count
    heads_here = offset_bias.shape[1]
    head_width = heads_here * HD
    reach = KR // 2
    scale = HD ** (-0.5)
    columns = jnp.arange(GRID_W, dtype=jnp.int32)
    col_first = jnp.clip(columns - KC // 2, 0, GRID_W - KC)
    col_inside = (columns[None, :] >= col_first[:, None]) & (
        columns[None, :] < col_first[:, None] + KC
    )
    col_offset = jnp.clip(columns[None, :] - columns[:, None], 1 - KC, KC - 1) + KC - 1
    col_onehot = (
        jnp.arange(2 * KC - 1, dtype=jnp.int32)[:, None, None] == col_offset[None, :, :]
    ).astype(jnp.float32)
    first_row = sp_index * local_rows
    own_rows = first_row + jnp.arange(local_rows, dtype=jnp.int32)
    row_first = jnp.clip(own_rows - reach, 0, grid_rows - KR)
    band_start = row_first - first_row + reach
    row_offset = (
        row_first[:, None] + jnp.arange(KR, dtype=jnp.int32)[None, :] - own_rows[:, None] + KR - 1
    )
    row_onehot = (
        row_offset[:, :, None] == jnp.arange(2 * KR - 1, dtype=jnp.int32)[None, None, :]
    ).astype(jnp.float32)
    qkv_weight = jnp.concatenate([w_query, w_key, w_value], axis=2)
    residual = lax.all_to_all(tokens, "sp", split_axis=1, concat_axis=0, tiled=True)
    width = residual.shape[1]
    features = width * sp_count
    for layer_index in range(LAYERS):
        wide = residual.astype(jnp.float32)
        squares = lax.psum_scatter(
            jnp.sum(wide * wide, axis=-1, keepdims=True), "sp", scatter_dimension=0, tiled=True
        )
        inverse = lax.rsqrt(squares / features + norm_eps)
        gain = lax.dynamic_slice_in_dim(norm_gain[layer_index], sp_index * width, width, 0)
        gained = (wide * gain.astype(jnp.float32)).astype(jnp.bfloat16)
        partial = jnp.dot(gained, qkv_weight[layer_index], preferred_element_type=jnp.float32)
        mine = lax.psum_scatter(
            partial.astype(jnp.bfloat16), "sp", scatter_dimension=0, tiled=True
        )
        mine = (mine.astype(jnp.float32) * inverse).astype(jnp.bfloat16)
        queries = mine[:, :head_width].reshape(local_rows, GRID_W, heads_here, HD)
        key_values = mine[:, head_width:].reshape(local_rows, GRID_W, 2 * head_width)
        padded = with_halo(key_values, (("sp", 0),), reach)
        bands = jax.vmap(lambda band_begin: lax.dynamic_slice_in_dim(padded, band_begin, KR, 0))(
            band_start
        )
        band_keys = bands[..., :head_width].reshape(local_rows, KR, GRID_W, heads_here, HD)
        band_values = bands[..., head_width:].reshape(local_rows, KR, GRID_W, heads_here, HD)
        col_bias = jnp.einsum(
            "hro,oqk->hrqk", offset_bias[layer_index], col_onehot, precision=lax.Precision.HIGHEST
        )
        full_bias = jnp.einsum(
            "ijr,hrqk->hiqjk", row_onehot, col_bias, precision=lax.Precision.HIGHEST
        )
        scores = jnp.einsum(
            "iqhd,ijkhd->hiqjk", queries, band_keys, preferred_element_type=jnp.float32
        )
        scores = scores * scale + full_bias
        scores = jnp.where(col_inside[None, None, :, None, :], scores, -jnp.inf)
        flattened = scores.reshape(heads_here, local_rows, GRID_W, KR * GRID_W)
        weights = jax.nn.softmax(flattened, axis=-1).astype(jnp.bfloat16)
        weights = weights.reshape(heads_here, local_rows, GRID_W, KR, GRID_W)
        attended = jnp.einsum(
            "hiqjk,ijkhd->iqhd", weights, band_values, preferred_element_type=jnp.float32
        )
        attended = attended.astype(jnp.bfloat16).reshape(tok_rows, head_width)
        every = lax.all_gather(attended, "sp", axis=0, tiled=True)
        share = jnp.dot(every, w_out[layer_index], preferred_element_type=jnp.float32)
        branch = lax.psum(share.astype(jnp.bfloat16), "tp").astype(jnp.float32)
        residual = (residual.astype(jnp.float32) + branch).astype(jnp.bfloat16)
    return lax.all_to_all(residual, "sp", split_axis=0, concat_axis=1, tiled=True)


MESH = pl.DeviceIdType.MESH
VMEM_MOST = 60 * 2**20
CHUNK = 128
PIECE = 64
LAG = 2


def greet(peers):
    barrier = pltpu.get_barrier_semaphore()
    for axis, index in peers:
        pl.semaphore_signal(barrier, inc=1, device_id={axis: index}, device_id_type=MESH)
    pl.semaphore_wait(barrier, len(peers))


def remote(src, dst, send, recv, axis, index):
    return pltpu.make_async_remote_copy(
        src_ref=src, dst_ref=dst, send_sem=send, recv_sem=recv,
        device_id={axis: index}, device_id_type=MESH,
    )


def span(start, size):
    return pl.ds(pl.multiple_of(start, size), size)


def spread_kernel(n, tok_ref, x_ref, send, recv, far_send, far_recv):
    me, t = lax.axis_index("sp"), lax.axis_index("tp")
    half = lax.rem(t, 2)
    partner = t + 1 - 2 * half
    rows, width = tok_ref.shape[0], tok_ref.shape[1] // n
    part = width // 2
    greet([("sp", lax.rem(me + k, n)) for k in range(1, n)] + [("tp", partner)])
    lanes = span(half * part, part)
    sent = []
    for k in range(1, n):
        to = lax.rem(me + k, n)
        copy = remote(
            tok_ref.at[:, span(to * width + half * part, part)],
            x_ref.at[span(me * rows, rows), lanes],
            send.at[k - 1], recv.at[k - 1], "sp", to,
        )
        copy.start()
        sent.append(copy)
    x_ref[span(me * rows, rows), :] = tok_ref[:, span(me * width, width)]
    passed = []
    for k in range(1, n):
        source = lax.rem(me + n - k, n)
        sent[k - 1].wait_recv()
        here = x_ref.at[span(source * rows, rows), lanes]
        copy = remote(here, here, far_send.at[k - 1], far_recv.at[k - 1], "tp", partner)
        copy.start()
        passed.append(copy)
    for k in range(n - 1):
        sent[k].wait_send()
        passed[k].wait()


def project_kernel(
    n, layer, features, x_ref, gain_ref, wq_ref, wk_ref, wv_ref, out_ref,
    gained, inbox, outbox, acc, sq_own, sq_in, inverse,
    send, recv, sq_send, sq_recv,
):
    me = lax.axis_index("sp")
    tokens, width = x_ref.shape
    cols = wq_ref.shape[1] // 2
    pieces = tokens // PIECE
    greet([("sp", lax.rem(me + k, n)) for k in range(1, n)])
    gain = gain_ref[pl.ds(layer, 1), span(me * width, width)].astype(jnp.float32)
    ones = jnp.ones((8, width), jnp.float32)

    @pl.loop(0, tokens // CHUNK)
    def _(i):
        rows = span(i * CHUNK, CHUNK)
        wide = x_ref[rows, :].astype(jnp.float32)
        gained[rows, :] = (wide * gain).astype(jnp.bfloat16)
        sq_own[:, rows] = lax.dot_general(
            ones, wide * wide, (((1,), (1,)), ((), ())),
            precision=lax.Precision.HIGHEST, preferred_element_type=jnp.float32,
        )

    ends = (n - 1, 0)
    for e, end in enumerate(ends):
        @pl.when(me != end)
        def _(e=e, end=end):
            remote(sq_own, sq_in.at[me], sq_send.at[e], sq_recv.at[me], "sp", end).start()

    at_end = (me == 0) | (me == n - 1)

    @pl.when(at_end)
    def _():
        for k in range(1, n):
            source = lax.rem(me + k, n)
            remote(sq_own, sq_in.at[source], sq_send.at[0], sq_recv.at[source], "sp", source).wait_recv()
        sq_in[me] = sq_own[...]

        @pl.loop(0, tokens // CHUNK)
        def _(i):
            rows = span(i * CHUNK, CHUNK)
            total = sq_in[0, :, rows]
            for k in range(1, n):
                total = total + sq_in[k, :, rows]
            scaled = lax.rsqrt(total / features + norm_eps)
            inverse[rows, :] = jnp.concatenate([scaled] * (CHUNK // 8), axis=0).T

    def flow(way, piece):
        place = me if way == 0 else n - 1 - me
        after = me + 1 if way == 0 else me - 1
        rows = span(piece * PIECE, PIECE)
        lo = (1 - way) * cols
        for j, w_ref in enumerate((wq_ref, wk_ref, wv_ref)):
            acc[:, j * cols:(j + 1) * cols] = jnp.dot(
                gained[rows, :], w_ref[:, lo:lo + cols], preferred_element_type=jnp.float32
            )

        def copy():
            return remote(
                outbox.at[way, rows, :], inbox.at[way, rows, :],
                send.at[way, piece], recv.at[way, piece], "sp", after,
            )

        @pl.when(place > 0)
        def _():
            copy().wait_recv()
            acc[...] += inbox[way, rows, :].astype(jnp.float32)

        @pl.when(place < n - 1)
        def _():
            outbox[way, rows, :] = acc[...].astype(jnp.bfloat16)
            copy().start()

        @pl.when(place == n - 1)
        def _():
            out_ref[rows, :] = (acc[...] * inverse[rows, :1]).astype(jnp.bfloat16)

    @pl.loop(0, pieces + (n - 1) * LAG)
    def _(step):
        for way in range(2):
            place = me if way == 0 else n - 1 - me
            piece = step - place * LAG

            @pl.when((piece >= 0) & (piece < pieces))
            def _(way=way, piece=piece):
                flow(way, piece)

    @pl.when(jnp.logical_not(at_end))
    def _():
        out_ref[...] = jnp.zeros_like(out_ref)

    for e, end in enumerate(ends):
        @pl.when(me != end)
        def _(e=e, end=end):
            remote(sq_own, sq_in.at[me], sq_send.at[e], sq_recv.at[me], "sp", end).wait_send()

            @pl.loop(0, pieces)
            def _(i):
                rows = span(i * PIECE, PIECE)
                remote(
                    outbox.at[e, rows, :], inbox.at[e, rows, :],
                    send.at[e, i], recv.at[e, i], "sp", end,
                ).wait_send()


def attend_kernel(heads, rows, scale, mine_ref, bias_ref, out_ref):
    cols = heads * HD
    for h in range(heads):
        for r in range(rows):
            first = min(max(r - KR // 2, 0), rows - KR)
            q = mine_ref[r * GRID_W:(r + 1) * GRID_W, h * HD:(h + 1) * HD]
            band = slice(first * GRID_W, (first + KR) * GRID_W)
            k = mine_ref[band, cols + h * HD:cols + (h + 1) * HD]
            v = mine_ref[band, 2 * cols + h * HD:2 * cols + (h + 1) * HD]
            scores = lax.dot_general(
                q, k, (((1,), (1,)), ((), ())), preferred_element_type=jnp.float32
            )
            scores = scores * scale + bias_ref[h, first - r + KR - 1]
            scores = jnp.exp(scores - jnp.max(scores, axis=-1, keepdims=True))
            weights = scores / jnp.sum(scores, axis=-1, keepdims=True)
            out = jnp.dot(weights.astype(jnp.bfloat16), v, preferred_element_type=jnp.float32)
            out_ref[r * GRID_W:(r + 1) * GRID_W, h * HD:(h + 1) * HD] = out.astype(jnp.bfloat16)


def combine_kernel(
    n, m, last, att_ref, x_ref, w_ref, out_ref,
    box, give, take, pair, cross_in, fresh,
    send, recv, give_s, give_r, cross_s, cross_r, fresh_s, fresh_r, far_s, far_r,
):
    me, t = lax.axis_index("sp"), lax.axis_index("tp")
    half = lax.rem(t, 2)
    partner = t + 1 - 2 * half
    cross = lax.rem(t + m // 2, m)
    tokens, width = x_ref.shape
    cols = att_ref.shape[1]
    part = width // 2
    chunks = tokens // CHUNK
    per = chunks // n
    lanes = span(half * part, part)
    other = span((1 - half) * part, part)
    greet(
        [("sp", lax.rem(me + k, n)) for k in range(1, n)] + [("tp", partner), ("tp", cross)]
    )

    def where(step):
        return span((lax.rem(step, n) * per + step // n) * CHUNK, CHUNK)

    def hop(way, step, source=None):
        rows = where(step)
        src = box.at[way, rows, :] if source is None else source.at[rows, :]
        after = me + 1 if way == 0 else me - 1
        return remote(src, box.at[way, rows, :], send.at[way, step], recv.at[way, step], "sp", after)

    for way, start in ((0, 0), (1, n - 1)):
        @pl.when(me == start)
        def _(way=way):
            @pl.loop(0, chunks)
            def _(i):
                hop(way, i, att_ref).start()
            box[way] = att_ref[...]

    def onward(way, step):
        place = me if way == 0 else n - 1 - me

        @pl.when(place > 0)
        def _():
            hop(way, step).wait_recv()

            @pl.when(place < n - 1)
            def _():
                hop(way, step).start()

    def forward(step):
        @pl.when(me < n // 2)
        def _():
            onward(0, step)
            onward(1, step)

        @pl.when(me >= n // 2)
        def _():
            onward(1, step)
            onward(0, step)

    def give_copy(step):
        rows = where(step)
        return remote(give.at[rows, :], take.at[rows, :], give_s.at[step], give_r.at[step], "tp", partner)

    def cross_copy(step):
        rows = where(step)
        return remote(
            pair.at[rows, :], cross_in.at[rows, :], cross_s.at[step], cross_r.at[step], "tp", cross
        )

    def multiply(step):
        rows = where(step)

        def share(at):
            return jnp.dot(
                box[0, rows, :], w_ref[:cols, at], preferred_element_type=jnp.float32
            ) + jnp.dot(box[1, rows, :], w_ref[cols:, at], preferred_element_type=jnp.float32)

        give[rows, :] = share(other).astype(jnp.bfloat16)
        give_copy(step).start()
        pair[rows, :] = share(lanes).astype(jnp.bfloat16)

    def meet(step):
        rows = where(step)
        give_copy(step).wait_recv()
        pair[rows, :] = (
            pair[rows, :].astype(jnp.float32) + take[rows, :].astype(jnp.float32)
        ).astype(jnp.bfloat16)
        cross_copy(step).start()

    def fresh_copy(step):
        rows = where(step)
        if not last:
            return remote(
                fresh.at[rows, :], out_ref.at[rows, lanes], fresh_s.at[step], fresh_r.at[step], "tp", partner
            )
        return remote(
            fresh.at[rows, :],
            out_ref.at[span(step // n * CHUNK, CHUNK), span(me * width + half * part, part)],
            fresh_s.at[step], fresh_r.at[me, step // n], "sp", lax.rem(step, n),
        )

    def finish(step):
        rows = where(step)
        cross_copy(step).wait_recv()
        branch = pair[rows, :].astype(jnp.float32) + cross_in[rows, :].astype(jnp.float32)
        new = (x_ref[rows, lanes].astype(jnp.float32) + branch).astype(jnp.bfloat16)
        if not last:
            fresh[rows, :] = new
            fresh_copy(step).start()
            out_ref[rows, lanes] = new
            return

        @pl.when(lax.rem(step, n) == me)
        def _():
            out_ref[span(step // n * CHUNK, CHUNK), span(me * width + half * part, part)] = new

        @pl.when(lax.rem(step, n) != me)
        def _():
            fresh[rows, :] = new
            fresh_copy(step).start()

    stages = ((forward, 0), (multiply, 1), (meet, 2), (finish, 4))

    @pl.loop(0, chunks + 4)
    def _(step):
        for stage, late in stages:
            at = step - late

            @pl.when((at >= 0) & (at < chunks))
            def _(stage=stage, at=at):
                stage(at)

    if last:
        def far_copy(source, q):
            here = out_ref.at[span(q * CHUNK, CHUNK), span(source * width + half * part, part)]
            return remote(here, here, far_s.at[source, q], far_r.at[source, q], "tp", partner)

        for q in range(per):
            for k in range(n):
                source = lax.rem(me + k, n)
                if k > 0:
                    here = out_ref.at[span(q * CHUNK, CHUNK), span(source * width + half * part, part)]
                    remote(
                        here, here, far_s.at[source, q], fresh_r.at[source, q], "sp", source
                    ).wait_recv()
                far_copy(source, q).start()
        for q in range(per):
            for k in range(n):
                source = lax.rem(me + k, n)
                there = out_ref.at[span(q * CHUNK, CHUNK), span(source * width + (1 - half) * part, part)]
                remote(there, there, far_s.at[source, q], far_r.at[source, q], "tp", partner).wait_recv()
                far_copy(source, q).wait_send()

    @pl.loop(0, chunks)
    def _(i):
        give_copy(i).wait_send()
        cross_copy(i).wait_send()
        if not last:
            rows = where(i)
            fresh_copy(i).wait_send()
            remote(
                fresh.at[rows, :], out_ref.at[rows, other], fresh_s.at[i], fresh_r.at[i], "tp", partner
            ).wait_recv()
        else:
            @pl.when(lax.rem(i, n) != me)
            def _():
                fresh_copy(i).wait_send()
        for way, end in ((0, n - 1), (1, 0)):
            @pl.when(me != end)
            def _(way=way):
                hop(way, i).wait_send()


def vmem():
    return pl.BlockSpec(memory_space=pltpu.VMEM)


def of_layer(array, layer):
    rest = array.shape[1:]
    return pl.BlockSpec((None, *rest), lambda i: (layer, *(0 for _ in rest)))


def params(identity):
    return pltpu.CompilerParams(
        collective_id=identity, has_side_effects=True, vmem_limit_bytes=VMEM_MOST
    )


def staged(tokens, norm_gain, w_query, w_key, w_value, w_out, offset_bias):
    n, m = lax.axis_size("sp"), lax.axis_size("tp")
    me = lax.axis_index("sp")
    own, features = tokens.shape
    width, total = features // n, own * n
    grid_rows = total // GRID_W
    heads = offset_bias.shape[1] // 2
    cols = heads * HD
    dma = pltpu.SemaphoreType.DMA
    bf16, f32 = jnp.bfloat16, jnp.float32

    columns = jnp.arange(GRID_W, dtype=jnp.int32)
    col_first = jnp.clip(columns - KC // 2, 0, GRID_W - KC)
    inside = (columns[None, :] >= col_first[:, None]) & (columns[None, :] < col_first[:, None] + KC)
    offset = jnp.clip(columns[None, :] - columns[:, None], 1 - KC, KC - 1) + KC - 1
    onehot = (
        jnp.arange(2 * KC - 1, dtype=jnp.int32)[:, None, None] == offset[None, :, :]
    ).astype(f32)
    table = lax.dynamic_slice_in_dim(offset_bias, jnp.where(me == n - 1, heads, 0), heads, 1)
    table = jnp.stack([table[:, :, a:a + KR] for a in range(KR)], axis=2)
    bias = jnp.einsum("lhajo,oqk->lhaqjk", table, onehot, precision=lax.Precision.HIGHEST)
    bias = jnp.where(inside[:, None, :], bias, -jnp.inf)
    bias = bias.reshape(LAYERS, heads, KR, GRID_W, KR * GRID_W)

    x = pl.pallas_call(
        functools.partial(spread_kernel, n),
        out_shape=jax.ShapeDtypeStruct((total, width), bf16),
        in_specs=[vmem()],
        grid=(1,),
        out_specs=vmem(),
        scratch_shapes=[dma((n - 1,))] * 4,
        compiler_params=params(1),
        name="spread",
    )(tokens)
    pieces, chunks = total // PIECE, total // CHUNK
    for layer in range(LAYERS):
        last = layer == LAYERS - 1
        mine = pl.pallas_call(
            functools.partial(project_kernel, n, layer, features),
            out_shape=jax.ShapeDtypeStruct((total, 3 * cols), bf16),
            in_specs=[vmem(), vmem()] + [of_layer(w, layer) for w in (w_query, w_key, w_value)],
            grid=(1,),
            out_specs=vmem(),
            scratch_shapes=[
                pltpu.VMEM((total, width), bf16),
                pltpu.VMEM((2, total, 3 * cols), bf16),
                pltpu.VMEM((2, total, 3 * cols), bf16),
                pltpu.VMEM((PIECE, 3 * cols), f32),
                pltpu.VMEM((8, total), f32),
                pltpu.VMEM((n, 8, total), f32),
                pltpu.VMEM((total, CHUNK), f32),
                dma((2, pieces)), dma((2, pieces)), dma((2,)), dma((n,)),
            ],
            compiler_params=params(2 + 2 * layer),
            name="project",
        )(x, norm_gain, w_query, w_key, w_value)
        attended = pl.pallas_call(
            functools.partial(attend_kernel, heads, grid_rows, HD ** (-0.5)),
            out_shape=jax.ShapeDtypeStruct((total, cols), bf16),
            in_specs=[vmem(), of_layer(bias, layer)],
            grid=(1,),
            out_specs=vmem(),
            compiler_params=pltpu.CompilerParams(vmem_limit_bytes=VMEM_MOST),
            name="attend",
        )(mine, bias)
        x = pl.pallas_call(
            functools.partial(combine_kernel, n, m, last),
            out_shape=jax.ShapeDtypeStruct((own, features) if last else (total, width), bf16),
            in_specs=[vmem(), vmem(), of_layer(w_out, layer)],
            grid=(1,),
            out_specs=vmem(),
            scratch_shapes=[
                pltpu.VMEM((2, total, cols), bf16),
                *[pltpu.VMEM((total, width // 2), bf16)] * 5,
                dma((2, chunks)), dma((2, chunks)),
                *[dma((chunks,))] * 4,
                dma((chunks,)),
                dma((n, chunks // n)) if last else dma((chunks,)),
                dma((n, chunks // n)), dma((n, chunks // n)),
            ],
            compiler_params=params(3 + 2 * layer),
            name="combine",
        )(attended, x, w_out)
    return x


def on_device(tokens, norm_gain, w_query, w_key, w_value, w_out, offset_bias):
    n, m = lax.axis_size("sp"), lax.axis_size("tp")
    own, features = tokens.shape
    total, width = own * n, features // n
    fits = total * (6 * width + 8 * w_query.shape[2]) * 2 < VMEM_MOST // 2
    even = offset_bias.shape[1] % 2 == 0 and m == 4 and n > 1
    if fits and even and own % CHUNK == 0 and width % 256 == 0:
        return staged(tokens, norm_gain, w_query, w_key, w_value, w_out, offset_bias)
    return general(tokens, norm_gain, w_query, w_key, w_value, w_out, offset_bias)


def solution(mesh):
    return jax.shard_map(
        on_device,
        mesh=mesh,
        in_specs=(
            P(("grp", "sp"), None),
            P(),
            P(None, "sp", "tp"),
            P(None, "sp", "tp"),
            P(None, "sp", "tp"),
            P(None, "tp", "sp"),
            P(None, "tp", None, None),
        ),
        out_specs=P(("grp", "sp"), None),
        check_vma=False,
    )
```
